32 devices in a mesh: sp: 8 (over z, x), tp: 4 (over y, core).
Axes of the slice: x: 2, y: 2, z: 4, core: 2. Of those that a mesh axis runs over, the one named last changes fastest.
Arguments:
- queries: bfloat16 [4096, 1024], P('sp', 'tp'), may hold values from -100 to 100
- keys: bfloat16 [4096, 256], P('sp', 'tp'), may hold values from -100 to 100
- values: bfloat16 [4096, 256], P('sp', 'tp'), may hold values from -6 to 6
- sink_logits: float32 [16], P('tp'), may hold values from 2 to 6
- stream: bfloat16 [4096, 2048], P(('sp', 'tp')), may hold values from -6 to 6
- out_proj: bfloat16 [1024, 2048], P('tp'), may hold values from -0.1875 to 0.1875
- norm_gain: float32 [2048], replicated, may hold values from 0.1 to 1.9
- routes: int32 [4096, 2], P(('sp', 'tp')), may hold values from 0 to 7, all different within a row; in each aligned block of 128 rows (0 to 127, 128 to 255, ...) at most 40 rows name the same one
- route_weights: float32 [4096, 2], P(('sp', 'tp')), may hold values from 0.2 to 1
- gate_proj: bfloat16 [8, 2048, 3584], P('sp', None, 'tp'), may hold values from -0.125 to 0.125
- up_proj: bfloat16 [8, 2048, 3584], P('sp', None, 'tp'), may hold values from -0.125 to 0.125
- down_proj: bfloat16 [8, 3584, 2048], P('sp', 'tp'), may hold values from -0.09375 to 0.09375
Outputs:
- layer_out: bfloat16 [4096, 2048], P(('sp', 'tp'))
The draws below stay inside these ranges and needn't reach their ends.
Inputs may be any that keep to these rules, and one draw needn't show every extreme that they name: `routes`: each row names two different experts. Among the rows of one device after the attention (aligned blocks of 128 rows) no expert is named more than 40 times.
All inputs are finite; a program needn't handle non-finite values.
Results may differ from the reference program's by a relative error of at most 0.009.
Values may be sent and summed in bfloat16 or wider, within the bound.
A program may use at most 128 MiB of HBM per device.

```python
import math
import jax
import jax.numpy as jnp
import numpy as np
from jax import lax

D = 2048
HQ = 16
HK = 4
DH = 64
WINDOW = 128
FF = 3584
TOK_DEV = 128
TOKENS = 4096
EXPERTS = 8
CAP = 40
N_SP = 8
N_TP = 4


def drawn_keys(key):
    base = jax.random.normal(jax.random.fold_in(key, 17), (TOKENS, HK * DH), jnp.float32)
    return jnp.clip(base, -100.0, 100.0)


def draw_keys(key, part):
    return drawn_keys(key).astype(jnp.bfloat16)


def draw_queries(key, part):
    base = jnp.clip(jax.random.normal(jax.random.fold_in(key, 29), (TOKENS, HQ * DH), jnp.float32), -6.0, 6.0)
    return jnp.clip(base, -100.0, 100.0).astype(jnp.bfloat16)


def level_of(rng, extent, shards, least, high):
    def one(axis_at, parts):
        heights = jax.random.uniform(jax.random.fold_in(jax.random.fold_in(rng, 6), axis_at), (parts,), jnp.float32, least / len(shards), high / len(shards))
        return jnp.repeat(jnp.exp(heights), extent[axis_at] // parts).reshape((-1,) + (1,) * (len(extent) - axis_at - 1))

    factor_of = one(*shards[0])
    for cut in shards[1:]:
        factor_of = factor_of * one(*cut)
    return factor_of


def shared_out(key, own, number, rows, number_of, top, reach, slope):
    order = jax.random.permutation(key, number_of)
    crowded, common = shares(number_of, rows * top, reach, slope, True), shares(number_of, rows * top, reach, slope, False)
    places = jnp.arange(number_of)

    def named(lengths, offset_by):
        used = int((lengths > 0).sum())
        fixed = max(1, used // 4)
        passed = fixed + (places - fixed + offset_by * (used - fixed)) % max(1, number_of - fixed)
        return jnp.zeros((number_of,), jnp.int32).at[order[jnp.where(places < fixed, places, passed)]].set(jnp.asarray(lengths, jnp.int32))

    lengths = jnp.where(number % 4 == 0, named(crowded, number // 4), named(common, number - number // 4 - 1))
    mixed = jax.random.permutation(jax.random.fold_in(own, 3), number_of)
    giver, receiver = mixed[0:number_of // 2 * 2:2], mixed[1:number_of // 2 * 2:2]
    room = jnp.minimum(lengths[giver] - 1, reach - lengths[receiver]) // 2
    room = jnp.where((giver == order[0]) | (receiver == order[0]) | (lengths[receiver] == 0), 0, jnp.maximum(room, 0))
    passed = jax.random.randint(jax.random.fold_in(own, 4), (number_of // 2,), 0, 1 << 20) % (room + 1)
    lengths = lengths.at[giver].add(-passed).at[receiver].add(passed)
    labels = jnp.searchsorted(jnp.cumsum(lengths), jnp.arange(rows * top), side="right").astype(jnp.int32)
    grid = labels.reshape(top, rows).T
    grid = grid[jax.random.permutation(jax.random.fold_in(own, 1), rows)]
    offset_by = jax.random.randint(jax.random.fold_in(own, 2), (rows, 1), 0, top)
    return jnp.take_along_axis(grid, (jnp.arange(top)[None, :] + offset_by) % top, axis=1)


def shares(number_of, total, bound, lean, full):
    portions = [(1 << 20) // math.isqrt(standing ** lean) + 1 for standing in range(1, number_of + 1)]
    largest = bound if full else min(bound, max(-(-total // number_of), total * portions[0] // sum(portions)))
    least = 1 if total - largest >= number_of - 1 else 0
    given, rest = [largest] + [least] * (number_of - 1), total - largest - least * (number_of - 1)
    while rest > 0:
        movable = [i for i in range(1, number_of) if given[i] < largest] or [i for i in range(1, number_of) if given[i] < bound]
        mass, budget = sum([portions[i] for i in movable]), rest
        for i in movable:
            more = min(bound - given[i], max(1, budget * portions[i] // mass), rest)
            given[i] = given[i] + more
            rest = rest - more
    return np.array(given)


def bell_draw(rng, shape, spread, most, cuts=(), held_as=jnp.bfloat16):
    gain = level_of(rng, shape, cuts, -0.22, 0.18) if cuts else 1.0
    entries = jax.random.normal(rng, shape, jnp.float32) * spread * gain
    return jnp.minimum(jnp.maximum(entries, -most), most).astype(held_as)


def setup_inputs(seed: int = 0) -> dict:
    streams_of = jax.random.split(jax.random.key(seed), 13)
    queries = draw_queries(jax.random.fold_in(streams_of[12], 71), 0)
    keys = draw_keys(jax.random.fold_in(streams_of[12], 71), 0)
    values = bell_draw(streams_of[2], (TOKENS, HK * DH), 1.0, 6.0, ((0, 8), (1, 4)))
    sink_logits = jnp.clip(2.0 + 4.0 * jax.random.uniform(streams_of[3], (HQ,), jnp.float32) ** level_of(streams_of[3], (HQ,), ((0, 4),), -0.2, 0.2), 2.0, 6.0)
    stream = bell_draw(streams_of[4], (TOKENS, D), 1.0, 6.0, ((0, 32),))
    out_proj = bell_draw(streams_of[5], (HQ * DH, D), (HQ * DH) ** -0.5, 0.1875, ((0, 4),))
    norm_gain = jnp.clip(1.0 + 0.18 * jax.random.normal(streams_of[6], (D,), jnp.float32), 0.1, 1.9)
    routes_keys = jax.random.split(jax.random.fold_in(streams_of[7], 1), TOKENS // TOK_DEV)
    routes_turns = jax.random.permutation(jax.random.fold_in(streams_of[7], 3), TOKENS // TOK_DEV)
    routes = jax.vmap(lambda own, number: shared_out(jax.random.fold_in(streams_of[7], 2), own, number, TOK_DEV, EXPERTS, 2, CAP, 2))(routes_keys, routes_turns).reshape((TOKENS, 2))
    route_weights = jnp.clip(0.2 + 0.8 * jax.random.uniform(streams_of[8], (TOKENS, 2), jnp.float32) ** level_of(streams_of[8], (TOKENS, 2), ((0, 32),), -0.2, 0.2), 0.2, 1.0)
    gate_proj = bell_draw(streams_of[9], (EXPERTS, D, FF), D ** -0.5, 0.125, ((0, 8), (2, 4)))
    up_proj = bell_draw(streams_of[10], (EXPERTS, D, FF), D ** -0.5, 0.125, ((0, 8), (2, 4)))
    down_proj = bell_draw(streams_of[11], (EXPERTS, FF, D), FF ** -0.5, 0.09375, ((0, 8), (1, 4)))
    return {"queries": queries, "keys": keys, "values": values, "sink_logits": sink_logits, "stream": stream, "out_proj": out_proj, "norm_gain": norm_gain, "routes": routes, "route_weights": route_weights, "gate_proj": gate_proj, "up_proj": up_proj, "down_proj": down_proj}


EPSILON = 1e-06

def attention(queries, keys, values, sink_logits):
    blocks = TOKENS // WINDOW
    group = HQ // HK
    query_blocks = queries.astype(jnp.float32).reshape(blocks, WINDOW, HK, group, DH)

    def banded(source):
        shaped = source.astype(jnp.float32).reshape(blocks, WINDOW, HK, DH)
        earlier = jnp.concatenate([jnp.zeros((1, WINDOW, HK, DH), jnp.float32), shaped[:-1]], axis=0)
        return jnp.concatenate([earlier, shaped], axis=1)
    key_band = banded(keys)
    value_band = banded(values)
    scores = jnp.einsum('nqkgd,nskd->nkgqs', query_blocks, key_band) * DH ** (-0.5)
    query_pos = jnp.arange(WINDOW, dtype=jnp.int32)[:, None] + WINDOW
    key_pos = jnp.arange(2 * WINDOW, dtype=jnp.int32)[None, :]
    distance = query_pos - key_pos
    key_abs = (jnp.arange(blocks, dtype=jnp.int32) * WINDOW - WINDOW)[:, None] + jnp.arange(2 * WINDOW, dtype=jnp.int32)[None, :]
    allowed = ((distance >= 0) & (distance < WINDOW))[None] & (key_abs >= 0)[:, None, :]
    logits = jnp.where(allowed[:, None, None], scores, -jnp.inf)
    sink_part = sink_logits.astype(jnp.float32).reshape(HK, group)[None, :, :, None]
    highest = jnp.maximum(lax.optimization_barrier(jnp.max(logits, axis=-1)), sink_part)
    expo = jnp.exp(logits - highest[..., None])
    denominator = lax.optimization_barrier(jnp.sum(expo, axis=-1)) + jnp.exp(sink_part - highest)
    weights = (expo / denominator[..., None]).astype(jnp.bfloat16)
    mixed_heads = jnp.einsum('nkgqs,nskd->nqkgd', weights.astype(jnp.float32), value_band)
    return mixed_heads.reshape(TOKENS, HQ * DH).astype(jnp.bfloat16)

def reference(queries, keys, values, sink_logits, stream, out_proj, norm_gain, routes, route_weights, gate_proj, up_proj, down_proj):
    attended = attention(queries, keys, values, sink_logits)
    mixed = stream.astype(jnp.float32) + jnp.dot(attended, out_proj, preferred_element_type=jnp.float32)
    scale = lax.rsqrt(lax.optimization_barrier(jnp.mean(mixed * mixed, axis=-1, keepdims=True)) + EPSILON)
    normed = (mixed * scale * norm_gain.astype(jnp.float32)).astype(jnp.bfloat16)
    slot_count = N_SP * N_TP * CAP
    ff_slice = FF // N_TP
    positions = jnp.arange(TOKENS, dtype=jnp.int32)

    def one_expert(running, inputs):
        gate_w, up_w, down_w, expert_id = inputs
        hit = routes == expert_id
        token_weight = lax.optimization_barrier(jnp.sum(jnp.where(hit, route_weights, jnp.float32(0.0)), axis=1))
        sort_key = jnp.where(jnp.any(hit, axis=1), positions, positions + TOKENS)
        picked = jnp.argsort(sort_key)[:slot_count].astype(jnp.int32)
        rows = normed[picked]
        gate_part = jnp.dot(rows, gate_w, preferred_element_type=jnp.float32)
        up_part = jnp.dot(rows, up_w, preferred_element_type=jnp.float32)
        hidden = (jax.nn.silu(gate_part) * up_part).astype(jnp.bfloat16)
        summed = jnp.zeros((slot_count, D), jnp.float32)
        for slice_index in range(N_TP):
            partial_value = jnp.dot(hidden[:, slice_index * ff_slice:(slice_index + 1) * ff_slice], down_w[slice_index * ff_slice:(slice_index + 1) * ff_slice], preferred_element_type=jnp.float32).astype(jnp.bfloat16)
            partial_value = lax.optimization_barrier(partial_value)
            summed = summed + partial_value.astype(jnp.float32)
        expert_out = summed.astype(jnp.bfloat16).astype(jnp.float32)
        running = running.at[picked].add(token_weight[picked][:, None] * expert_out)
        return (running, None)
    start = jnp.zeros((TOKENS, D), jnp.float32)
    routed, _ = lax.scan(one_expert, start, (gate_proj, up_proj, down_proj, jnp.arange(EXPERTS, dtype=jnp.int32)))
    return (mixed + routed).astype(jnp.bfloat16)
```

```python
import functools

import jax
import jax.numpy as jnp
from jax import lax
from jax.experimental import pallas as pl
from jax.experimental.pallas import tpu as pltpu
from jax.sharding import PartitionSpec as P

DH = 64
WINDOW = 128
EPSILON = 1e-06
MESH = pl.DeviceIdType.MESH
F32 = jnp.float32
BF16 = jnp.bfloat16


def dot(a, b, dims=((1,), (0,))):
    return lax.dot_general(a, b, (dims, ((), ())), preferred_element_type=F32)


def greet(n, sp, partners):
    barrier = pltpu.get_barrier_semaphore()

    def hello(d, carry):
        pl.semaphore_signal(
            barrier, inc=1, device_id={"sp": lax.rem(sp + d, n)}, device_id_type=MESH
        )
        return carry

    lax.fori_loop(1, n, hello, 0)
    for t in partners:
        pl.semaphore_signal(barrier, inc=1, device_id={"tp": t}, device_id_type=MESH)
    pl.semaphore_wait(barrier, n - 1 + len(partners))


def slots_of(n, routes_t):
    rows = routes_t.shape[1]
    ids = lax.broadcasted_iota(jnp.int32, (n, rows), 0)
    hit = (routes_t[0:1, :] == ids) | (routes_t[1:2, :] == ids)
    before = lax.broadcasted_iota(jnp.int32, (rows, rows), 0) < lax.broadcasted_iota(
        jnp.int32, (rows, rows), 1
    )
    rank = dot(hit.astype(F32).astype(BF16), before.astype(F32).astype(BF16))
    return jnp.where(hit, rank, -1.0)


def picker_of(slot_row, cap):
    c = lax.broadcasted_iota(jnp.int32, (cap, slot_row.shape[1]), 0).astype(F32)
    return (slot_row == c).astype(F32).astype(BF16)


def front(
    n,
    q_ref,
    kv_ref,
    sink_ref,
    wo_ref,
    stream_ref,
    gain_ref,
    routes_ref,
    gate_ref,
    up_ref,
    down_ref,
    rows_ref,
    mixed_ref,
    gate_out,
    up_out,
    down_out,
    tail,
    wo_peer,
    att,
    att_peer,
    part_out,
    part_in,
    outgoing,
    normed,
    slots,
    one_send,
    one_recv,
    part_send,
    part_recv,
    out_send,
    out_recv,
    fwd_send,
    fwd_recv,
):
    sp = lax.axis_index("sp")
    tp = lax.axis_index("tp")
    lo = lax.rem(tp, 2)
    hi = tp // 2
    pair = 2 * hi + 1 - lo
    cross = 2 * (1 - hi) + lo
    tok = q_ref.shape[0]
    heads = q_ref.shape[1] // DH
    rows = stream_ref.shape[0]
    width = stream_ref.shape[1]
    cap = outgoing.shape[1]
    greet(n, sp, (pair, cross))

    def remote(src, dst, s, r, **where):
        return pltpu.make_async_remote_copy(
            src_ref=src, dst_ref=dst, send_sem=s, recv_sem=r, device_id=where, device_id_type=MESH
        )

    tail_copy = remote(
        kv_ref.at[pl.ds(tok - WINDOW, WINDOW)],
        tail,
        one_send.at[0],
        one_recv.at[0],
        sp=lax.rem(sp + 1, n),
    )
    tail_copy.start()
    wo_copy = remote(wo_ref, wo_peer, one_send.at[1], one_recv.at[1], tp=pair)
    wo_copy.start()

    slots[...] = slots_of(n, routes_ref[...])
    query = lax.broadcasted_iota(jnp.int32, (WINDOW, 2 * WINDOW), 0) + WINDOW
    key = lax.broadcasted_iota(jnp.int32, (WINDOW, 2 * WINDOW), 1)
    inside = (query - key >= 0) & (query - key < WINDOW)
    blocks = tok // WINDOW
    for b in list(range(1, blocks)) + [0]:
        if b == 0:
            tail_copy.wait()
            band = jnp.concatenate([tail[...], kv_ref[pl.ds(0, WINDOW), :]], axis=0)
            allowed = inside & ((key >= WINDOW) | (sp > 0))
        else:
            band = kv_ref[pl.ds((b - 1) * WINDOW, 2 * WINDOW), :]
            allowed = inside
        pieces = []
        kb, vb = band[:, :DH], band[:, DH:]
        qb = q_ref[pl.ds(b * WINDOW, WINDOW), :]
        for h in range(heads):
            score = dot(qb[:, h * DH : (h + 1) * DH], kb, ((1,), (1,))) * DH ** (-0.5)
            score = jnp.where(allowed, score, -jnp.inf)
            sink = sink_ref[h]
            top = jnp.maximum(jnp.max(score, axis=-1, keepdims=True), sink)
            expo = jnp.exp(score - top)
            denom = jnp.sum(expo, axis=-1, keepdims=True) + jnp.exp(sink - top)
            pieces.append(dot((expo / denom).astype(BF16), vb))
        att[pl.ds(b * WINDOW, WINDOW), :] = jnp.concatenate(pieces, axis=1).astype(BF16)

    att_copies = []
    for g in range(2):
        where = pl.multiple_of((2 * g + 1 - lo) * rows, rows)
        copy = remote(
            att.at[pl.ds(where, rows)],
            att_peer.at[g],
            one_send.at[2 + g],
            one_recv.at[2 + g],
            tp=pair,
        )
        copy.start()
        att_copies.append(copy)
    weight_copies = []
    for k, (src, dst) in enumerate(((gate_ref, gate_out), (up_ref, up_out), (down_ref, down_out))):
        copy = remote(src, dst, one_send.at[4 + k], one_recv.at[4 + k], tp=pair)
        copy.start()
        weight_copies.append(copy)
    wo_copy.wait()
    for copy in att_copies:
        copy.wait()

    chunk = width // 4
    part_copies = []
    mine = att[pl.ds(pl.multiple_of(cross * rows, rows), rows), :]
    theirs = att_peer[1 - hi]
    for k in range(4):
        cols = pl.ds(k * chunk, chunk)
        part_out[k] = (dot(mine, wo_ref[:, cols]) + dot(theirs, wo_peer[:, cols])).astype(BF16)
        copy = remote(part_out.at[k], part_in.at[k], part_send.at[k], part_recv.at[k], tp=cross)
        copy.start()
        part_copies.append(copy)
    mine = att[pl.ds(pl.multiple_of(tp * rows, rows), rows), :]
    theirs = att_peer[hi]
    for k in range(4):
        cols = pl.ds(k * chunk, chunk)
        mixed_ref[:, cols] = (
            stream_ref[:, cols].astype(F32)
            + dot(mine, wo_ref[:, cols])
            + dot(theirs, wo_peer[:, cols])
        )
    square = jnp.zeros((rows, 1), F32)
    for k in range(4):
        cols = pl.ds(k * chunk, chunk)
        part_copies[k].wait()
        value = mixed_ref[:, cols] + part_in[k].astype(F32)
        mixed_ref[:, cols] = value
        square = square + jnp.sum(value * value, axis=-1, keepdims=True)
    scale = lax.rsqrt(square / width + EPSILON)
    for k in range(4):
        cols = pl.ds(k * chunk, chunk)
        normed[:, cols] = (mixed_ref[:, cols] * scale * gain_ref[:, cols]).astype(BF16)

    def sent(d):
        e = lax.rem(sp + d, n)
        return remote(outgoing.at[e], rows_ref.at[0, sp], out_send.at[d], out_recv.at[d], sp=e)

    def arrival(d):
        s = lax.rem(sp + n - d, n)
        return remote(outgoing.at[s], rows_ref.at[0, s], out_send.at[d], out_recv.at[d], sp=s)

    def forward(d):
        s = lax.rem(sp + n - d, n)
        return remote(
            rows_ref.at[0, s], rows_ref.at[1, s], fwd_send.at[d], fwd_recv.at[d], tp=cross
        )

    def pick(e):
        picker = picker_of(slots[pl.ds(e, 1), :], cap)
        return dot(picker, normed[...]).astype(BF16)

    rows_ref[0, sp] = pick(sp)
    forward(0).start()

    def send(i, carry):
        e = lax.rem(sp + i, n)
        outgoing[e] = pick(e)
        sent(i).start()
        return carry

    lax.fori_loop(1, n, send, 0)

    def relay(d, carry):
        arrival(d).wait_recv()
        forward(d).start()
        return carry

    lax.fori_loop(1, n, relay, 0)

    def finish(d, carry):
        sent(d).wait_send()
        return carry

    lax.fori_loop(1, n, finish, 0)

    def finish_forward(d, carry):
        forward(d).wait()
        return carry

    lax.fori_loop(0, n, finish_forward, 0)
    for copy in weight_copies:
        copy.wait()


def back(
    n,
    partial_ref,
    mixed_ref,
    routes_ref,
    routes_t_ref,
    weights_ref,
    out_ref,
    peer,
    outgoing,
    returned,
    total,
    slots,
    pair_send,
    pair_recv,
    out_send,
    out_recv,
):
    sp = lax.axis_index("sp")
    tp = lax.axis_index("tp")
    lo = lax.rem(tp, 2)
    cross = 2 * (1 - tp // 2) + lo
    cap = outgoing.shape[1]
    greet(n, sp, (cross,))

    def remote(src, dst, s, r, **where):
        return pltpu.make_async_remote_copy(
            src_ref=src, dst_ref=dst, send_sem=s, recv_sem=r, device_id=where, device_id_type=MESH
        )

    def swap(d):
        s = lax.rem(sp + d, n)
        return remote(partial_ref.at[1, s], peer.at[s], pair_send.at[d], pair_recv.at[d], tp=cross)

    def sent(d):
        s = lax.rem(sp + d, n)
        return remote(outgoing.at[s], returned.at[sp], out_send.at[d], out_recv.at[d], sp=s)

    def arrival(d):
        e = lax.rem(sp + n - d, n)
        return remote(outgoing.at[e], returned.at[e], out_send.at[d], out_recv.at[d], sp=e)

    def begin(i, carry):
        swap(lax.rem(i, n)).start()
        return carry

    lax.fori_loop(1, n + 1, begin, 0)
    slots[...] = slots_of(n, routes_t_ref[...])
    total[...] = mixed_ref[...]

    def summed(s):
        return (partial_ref[0, s].astype(F32) + peer[s].astype(F32)).astype(BF16)

    def send(d, carry):
        swap(d).wait()
        s = lax.rem(sp + d, n)
        outgoing[s] = summed(s)
        sent(d).start()
        return carry

    lax.fori_loop(1, n, send, 0)
    swap(0).wait()
    returned[sp] = summed(sp)
    routes = routes_ref[...]
    weights = weights_ref[...]

    def add(e):
        picker = picker_of(slots[pl.ds(e, 1), :], cap)
        weight = jnp.sum(jnp.where(routes == e, weights, 0.0), axis=1, keepdims=True)
        total[...] += weight * dot(picker, returned[e], ((0,), (0,)))

    add(sp)

    def gather(d, carry):
        arrival(d).wait_recv()
        add(lax.rem(sp + n - d, n))
        return carry

    lax.fori_loop(1, n, gather, 0)

    def finish(d, carry):
        sent(d).wait_send()
        return carry

    lax.fori_loop(1, n, finish, 0)
    out_ref[...] = total[...].astype(BF16)


def on_device(
    queries,
    keys,
    values,
    sink_logits,
    stream,
    out_proj,
    norm_gain,
    routes,
    route_weights,
    gate_proj,
    up_proj,
    down_proj,
):
    n = lax.axis_size("sp")
    tok_sp, att_width = queries.shape
    rows, width = stream.shape
    capacity = max(2, (5 * rows + 2 * n - 1) // (2 * n))
    cap = -(-capacity // 8) * 8
    kv = jnp.concatenate([keys, values], axis=1)
    routes_t = routes.T
    gate, up, down = gate_proj[0], up_proj[0], down_proj[0]
    vmem = pl.BlockSpec(memory_space=pltpu.VMEM)
    smem = pl.BlockSpec(memory_space=pltpu.SMEM)
    anywhere = pl.BlockSpec(memory_space=pltpu.HBM)
    dma = pltpu.SemaphoreType.DMA
    like = jax.ShapeDtypeStruct
    arrived, mixed, gate_two, up_two, down_two = pl.pallas_call(
        functools.partial(front, n),
        out_shape=(
            like((2, n, cap, width), BF16),
            like((rows, width), F32),
            like(gate.shape, BF16),
            like(up.shape, BF16),
            like(down.shape, BF16),
        ),
        in_specs=[vmem, vmem, smem, vmem, vmem, vmem, vmem, anywhere, anywhere, anywhere],
        out_specs=(vmem, vmem, anywhere, anywhere, anywhere),
        scratch_shapes=[
            pltpu.VMEM((WINDOW, 2 * DH), BF16),
            pltpu.VMEM(out_proj.shape, BF16),
            pltpu.VMEM((tok_sp, att_width), BF16),
            pltpu.VMEM((2, rows, att_width), BF16),
            pltpu.VMEM((4, rows, width // 4), BF16),
            pltpu.VMEM((4, rows, width // 4), BF16),
            pltpu.VMEM((n, cap, width), BF16),
            pltpu.VMEM((rows, width), BF16),
            pltpu.VMEM((n, rows), F32),
            dma((7,)),
            dma((7,)),
            dma((4,)),
            dma((4,)),
            dma((n,)),
            dma((n,)),
            dma((n,)),
            dma((n,)),
        ],
        compiler_params=pltpu.CompilerParams(collective_id=0, has_side_effects=True),
        name="front",
    )(
        queries,
        kv,
        sink_logits,
        out_proj,
        stream,
        norm_gain.reshape(1, width),
        routes_t,
        gate,
        up,
        down,
    )
    expert_rows = arrived.reshape(2 * n * cap, width)

    def expert(g, u):
        gate_part = jnp.dot(expert_rows, g, preferred_element_type=F32)
        up_part = jnp.dot(expert_rows, u, preferred_element_type=F32)
        return (jax.nn.silu(gate_part) * up_part).astype(BF16)

    partial_value = jnp.dot(expert(gate, up), down, preferred_element_type=F32) + jnp.dot(
        expert(gate_two, up_two), down_two, preferred_element_type=F32
    )
    partial_value = partial_value.astype(BF16).reshape(2, n, cap, width)
    return pl.pallas_call(
        functools.partial(back, n),
        out_shape=like((rows, width), BF16),
        in_specs=[vmem] * 5,
        out_specs=vmem,
        scratch_shapes=[
            pltpu.VMEM((n, cap, width), BF16),
            pltpu.VMEM((n, cap, width), BF16),
            pltpu.VMEM((n, cap, width), BF16),
            pltpu.VMEM((rows, width), F32),
            pltpu.VMEM((n, rows), F32),
            dma((n,)),
            dma((n,)),
            dma((n,)),
            dma((n,)),
        ],
        compiler_params=pltpu.CompilerParams(collective_id=1, has_side_effects=True),
        name="back",
    )(partial_value, mixed, routes, routes_t, route_weights)


def solution(mesh):
    return jax.shard_map(
        on_device,
        mesh=mesh,
        in_specs=(
            P("sp", "tp"),
            P("sp", "tp"),
            P("sp", "tp"),
            P("tp"),
            P(("sp", "tp"), None),
            P("tp", None),
            P(),
            P(("sp", "tp"), None),
            P(("sp", "tp"), None),
            P("sp", None, "tp"),
            P("sp", None, "tp"),
            P("sp", "tp", None),
        ),
        out_specs=P(("sp", "tp"), None),
        check_vma=False,
    )
```
